32 devices in a mesh: sp: 8 (over z, x), tp: 4 (over y, core).
Axes of the slice: x: 2, y: 2, z: 4, core: 2. Of those that a mesh axis runs over, the one named last changes fastest.
Arguments:
- tokens: bfloat16 [1024, 2048], P('sp', 'tp'), may hold values from -6 to 6
- norm_gain: float32 [2048], replicated, may hold values from 0.1 to 1.9
- da_query: bfloat16 [2048, 1024], P(None, 'tp'), as said below
- da_key: bfloat16 [2048, 1024], P(None, 'tp'), may hold values from -0.125 to 0.125
- da_value: bfloat16 [2048, 1024], P(None, 'tp'), may hold values from -0.125 to 0.125
- mix_lambda: float32 [8], P('tp'), may hold values from 0.3 to 0.8
- attn_gain: float32 [128], replicated, may hold values from 0.1 to 1.9
- rec_query: bfloat16 [2048, 1024], P(None, 'tp'), may hold values from -0.125 to 0.125
- rec_forget_fwd: bfloat16 [2048, 1024], P(None, 'tp'), may hold values from -0.375 to 0.375
- rec_forget_bwd: bfloat16 [2048, 1024], P(None, 'tp'), may hold values from -0.375 to 0.375
- rec_value: bfloat16 [2048, 1024], P(None, 'tp'), may hold values from -0.125 to 0.125
- gate_gap: float32 [2, 1024], P(None, 'tp'), may hold values from 0.0009765625 to 0.12
- extra_decay: float32 [2, 1024, 8], P(None, 'sp', 'tp'), may hold values from -0.7 to 0
- init_state: float32 [2, 8, 128, 128], P(None, 'tp'), may hold values from -1.5 to 1.5
- rec_gain: float32 [128], replicated, may hold values from 0.1 to 1.9
- out_attn: bfloat16 [1024, 2048], P('tp'), may hold values from -0.125 to 0.125
- out_rec: bfloat16 [1024, 2048], P('tp'), may hold values from -0.125 to 0.125
Outputs:
- mixed: bfloat16 [1024, 2048], P(('sp', 'tp'))
The draws below stay inside these ranges and needn't reach their ends.
Inputs may be any that keep to these rules, and one draw needn't show every extreme that they name: `da_query`: entries lie within -240 / sqrt(2048) and 240 / sqrt(2048).
All inputs are finite; a program needn't handle non-finite values.
Results may differ from the reference program's by a relative error of at most 0.014.
The reference program's roundings to bfloat16 on the way count: a program that leaves them out, or rounds other values in their place, can miss the bound.
Values may be sent and summed in bfloat16 or wider, within the bound.
A program may use at most 128 MiB of HBM per device.

```python
import math
import jax
import jax.numpy as jnp
from jax import lax

D = 2048
DA_HEADS = 8
QK_DIM = 64
DA_VAL = 128
RECURRENT_HEADS = 8
HG_KEY = 128
HG_VAL = 128
SPAN = 64
TOK_DEV = 128
TOKEN_COUNT = 1024


def draw_da_query(key, part):
    spread = 1.8
    base = jnp.clip(jax.random.normal(key, (D, DA_HEADS * 2 * QK_DIM), jnp.float32), -6.0, 6.0)
    return (base * (spread / math.sqrt(D))).astype(jnp.bfloat16)


def draw_gate_gap(key, part):
    head_key, slow_key, fast_key = jax.random.split(jax.random.fold_in(key, 11), 3)
    chance = 0.5
    slow_heads = jax.random.uniform(head_key, (2, RECURRENT_HEADS, 1), jnp.float32) < chance
    slow_gap = jax.random.uniform(slow_key, (2, RECURRENT_HEADS, HG_KEY), jnp.float32, 1.0, 3.0) / TOKEN_COUNT
    fast_gap = jnp.exp(jax.random.uniform(fast_key, (2, RECURRENT_HEADS, HG_KEY), jnp.float32, math.log(0.04), math.log(0.12)))
    return jnp.where(slow_heads, slow_gap, fast_gap).reshape(2, RECURRENT_HEADS * HG_KEY).astype(jnp.float32)


def draw_extra_decay(key, part):
    rate_key, key_position, depth_key = jax.random.split(jax.random.fold_in(key, 23), 3)
    half_rows = max(TOK_DEV // 2, 1)
    block_count = TOKEN_COUNT // half_rows
    rates = jnp.exp(jax.random.uniform(rate_key, (2, block_count, 1, RECURRENT_HEADS), jnp.float32, math.log(0.3), math.log(3.0)))
    steady_decay = jnp.broadcast_to(-rates / TOKEN_COUNT, (2, block_count, half_rows, RECURRENT_HEADS)).reshape(2, TOKEN_COUNT, RECURRENT_HEADS)
    sudden_inputs = jax.random.uniform(key_position, (2, TOKEN_COUNT, RECURRENT_HEADS), jnp.float32) < 4.0 / TOKEN_COUNT
    decay_drops = jnp.log(jax.random.uniform(depth_key, (2, TOKEN_COUNT, RECURRENT_HEADS), jnp.float32, 0.5, 0.8))
    return jnp.where(sudden_inputs, decay_drops, steady_decay).astype(jnp.float32)


def block_scale(rng, dims, pieces, smallest, largest):
    loudness, own = 1.0, jax.random.fold_in(rng, 6)
    for position, blocks in pieces:
        draws = jnp.exp(jax.random.uniform(jax.random.fold_in(own, position), (blocks,), jnp.float32, smallest / len(pieces), largest / len(pieces)))
        loudness = loudness * jnp.repeat(draws, dims[position] // blocks).reshape([-1 if axis == position else 1 for axis in range(len(dims))])
    return loudness


def noise(key, extent, deviation, limit, pieces=(), kind=jnp.bfloat16):
    values = jax.random.normal(key, extent, jnp.float32) * deviation
    if len(pieces) > 0:
        values = block_scale(key, extent, pieces, -0.22, 0.18) * values
    return jnp.clip(values, min=-limit, max=limit).astype(kind)


def setup_inputs(seed: int = 0) -> dict:
    key_of = jax.random.split(jax.random.key(seed), 18)
    tokens = noise(key_of[0], (TOKEN_COUNT, D), 1.0, 6.0, ((0, 8), (1, 4)))
    norm_gain = jnp.clip(1.0 + 0.18 * jax.random.normal(key_of[1], (D,), jnp.float32), 0.1, 1.9)
    da_query = draw_da_query(jax.random.fold_in(key_of[17], 71), 0)
    da_key = noise(key_of[3], (D, DA_HEADS * 2 * QK_DIM), D ** -0.5, 0.125, ((1, 4),))
    da_value = noise(key_of[4], (D, DA_HEADS * DA_VAL), D ** -0.5, 0.125, ((1, 4),))
    mix_lambda = jnp.clip(0.3 + 0.5 * jax.random.uniform(key_of[5], (DA_HEADS,), jnp.float32) ** block_scale(key_of[5], (DA_HEADS,), ((0, 4),), -0.2, 0.2), 0.3, 0.8)
    attn_gain = jnp.clip(1.0 + 0.18 * jax.random.normal(key_of[6], (DA_VAL,), jnp.float32), 0.1, 1.9)
    rec_query = noise(key_of[7], (D, RECURRENT_HEADS * HG_KEY), D ** -0.5, 0.125, ((1, 4),))
    rec_forget_fwd = noise(key_of[8], (D, RECURRENT_HEADS * HG_KEY), (D // 8) ** -0.5, 0.375, ((1, 4),))
    rec_forget_bwd = noise(key_of[9], (D, RECURRENT_HEADS * HG_KEY), (D // 8) ** -0.5, 0.375, ((1, 4),))
    rec_value = noise(key_of[10], (D, RECURRENT_HEADS * HG_VAL), D ** -0.5, 0.125, ((1, 4),))
    gate_gap = draw_gate_gap(jax.random.fold_in(key_of[17], 71), 0)
    extra_decay = draw_extra_decay(jax.random.fold_in(key_of[17], 71), 0)
    init_state = noise(key_of[13], (2, RECURRENT_HEADS, HG_KEY, HG_VAL), (3.0 * TOKEN_COUNT ** -0.5), 1.5, ((1, 4),), jnp.float32)
    rec_gain = jnp.clip(1.0 + 0.18 * jax.random.normal(key_of[14], (HG_VAL,), jnp.float32), 0.1, 1.9)
    out_attn = noise(key_of[15], (DA_HEADS * DA_VAL, D), (DA_HEADS * DA_VAL + RECURRENT_HEADS * HG_VAL) ** -0.5, 0.125, ((0, 4),))
    out_rec = noise(key_of[16], (RECURRENT_HEADS * HG_VAL, D), (DA_HEADS * DA_VAL + RECURRENT_HEADS * HG_VAL) ** -0.5, 0.125, ((0, 4),))
    return {"tokens": tokens, "norm_gain": norm_gain, "da_query": da_query, "da_key": da_key, "da_value": da_value, "mix_lambda": mix_lambda, "attn_gain": attn_gain, "rec_query": rec_query, "rec_forget_fwd": rec_forget_fwd, "rec_forget_bwd": rec_forget_bwd, "rec_value": rec_value, "gate_gap": gate_gap, "extra_decay": extra_decay, "init_state": init_state, "rec_gain": rec_gain, "out_attn": out_attn, "out_rec": out_rec}


EPSILON = 1e-06
EXACT_PRECISION = lax.Precision.HIGHEST

def block_scan(query, key_in, values, log_decay, initial):
    length = query.shape[0]
    count = length // SPAN

    def split(array):
        return array.reshape((count, SPAN) + array.shape[1:])
    lower = jnp.tril(jnp.ones((SPAN, SPAN), jnp.float32))

    def one_step(carried_state, inputs):
        query_tile, key_tile, value_tile, g_block = inputs
        cumulative_decay = jnp.cumsum(g_block, axis=0)
        relative = cumulative_decay[:, None] - cumulative_decay[None, :]
        relative = jnp.where(lower[:, :, None, None] > 0, relative, -jnp.inf)
        score_matrix = jnp.einsum('ihk,ijhk,jhk->hij', query_tile, jnp.exp(relative), key_tile, precision=EXACT_PRECISION)
        output_rows = jnp.einsum('ujg,jga->uja', query_tile * jnp.exp(cumulative_decay), carried_state, precision=EXACT_PRECISION) + jnp.einsum('ots,sok->tok', score_matrix, value_tile, precision=EXACT_PRECISION)
        ending_state = cumulative_decay[-1]
        carried_state = jnp.exp(ending_state)[..., None] * carried_state + jnp.einsum('zds,zdx->dsx', key_tile * jnp.exp(ending_state[None] - cumulative_decay), value_tile, precision=EXACT_PRECISION)
        return (carried_state, output_rows)
    carried_state, output_rows = lax.scan(one_step, initial, (split(query), split(key_in), split(values), split(log_decay)))
    return (output_rows.reshape((length,) + output_rows.shape[2:]), carried_state)

def reference(tokens, norm_gain, da_query, da_key, da_value, mix_lambda, attn_gain, rec_query, rec_forget_fwd, rec_forget_bwd, rec_value, gate_gap, extra_decay, init_state, rec_gain, out_attn, out_rec):
    values = tokens.astype(jnp.float32)
    scaled = (values * norm_gain).astype(jnp.bfloat16)
    inv_rms = lax.rsqrt(lax.optimization_barrier(jnp.mean(values * values, axis=1, keepdims=True)) + EPSILON)

    def project(weight):
        return (jnp.dot(scaled, weight, preferred_element_type=jnp.float32) * inv_rms).astype(jnp.bfloat16)
    query_att = project(da_query).reshape(TOKEN_COUNT, DA_HEADS, 2, QK_DIM)
    key_att = project(da_key).reshape(TOKEN_COUNT, DA_HEADS, 2, QK_DIM).astype(jnp.float32)
    value_att = project(da_value).reshape(TOKEN_COUNT, DA_HEADS, DA_VAL).astype(jnp.float32)
    query_rows = math.gcd(TOKEN_COUNT, 256)
    query_blocks = query_att.reshape(TOKEN_COUNT // query_rows, query_rows, DA_HEADS, 2, QK_DIM)

    def attend(query_block):
        score_matrix = jnp.einsum('qhmd,khmd->hmqk', query_block.astype(jnp.float32), key_att) * QK_DIM ** (-0.5)
        maxima = lax.optimization_barrier(jnp.max(score_matrix, axis=3, keepdims=True))
        unnorm = jnp.exp(score_matrix - maxima)
        denoms = lax.optimization_barrier(jnp.sum(unnorm, axis=3))
        rounded = lax.optimization_barrier(unnorm.astype(jnp.bfloat16)).astype(jnp.float32)
        numerator = jnp.einsum('hmqk,khv->hmqv', rounded, value_att)
        ratio = numerator / denoms[..., None]
        diff = ratio[:, 0] - mix_lambda[:, None, None] * ratio[:, 1]
        normed = diff * lax.rsqrt(lax.optimization_barrier(jnp.mean(diff * diff, axis=-1, keepdims=True)) + EPSILON) * attn_gain
        return jnp.transpose(normed, (1, 0, 2)).astype(jnp.bfloat16)
    attn_out = lax.map(attend, query_blocks).reshape(TOKEN_COUNT, DA_HEADS * DA_VAL)

    def heads(array, width):
        return array.astype(jnp.float32).reshape(TOKEN_COUNT, RECURRENT_HEADS, width)
    rec_q = jax.nn.silu(heads(project(rec_query), HG_KEY)) * HG_KEY ** (-0.5)
    values_rec = heads(project(rec_value), HG_VAL)
    forgets = (project(rec_forget_fwd), project(rec_forget_bwd))
    outputs = []
    for direction in range(2):
        gap = gate_gap[direction].reshape(RECURRENT_HEADS, HG_KEY)
        key_in = gap * jax.nn.sigmoid(-heads(forgets[direction], HG_KEY))
        log_decay = jnp.log1p(-key_in) + extra_decay[direction][:, :, None]
        if direction == 0:
            result, unused = block_scan(rec_q, key_in, values_rec, log_decay, init_state[0])
        else:
            result, unused = block_scan(rec_q[::-1], key_in[::-1], values_rec[::-1], log_decay[::-1], init_state[1])
            result = result[::-1]
        outputs.append(result)
    rec_sum = outputs[0] + outputs[1]
    rec_normed = rec_sum * lax.rsqrt(lax.optimization_barrier(jnp.mean(rec_sum * rec_sum, axis=-1, keepdims=True)) + EPSILON) * rec_gain
    rec_out = rec_normed.reshape(TOKEN_COUNT, RECURRENT_HEADS * HG_VAL).astype(jnp.bfloat16)
    mixed = jnp.dot(attn_out, out_attn, preferred_element_type=jnp.float32) + jnp.dot(rec_out, out_rec, preferred_element_type=jnp.float32)
    return mixed.astype(jnp.bfloat16)
```

```python
import functools

import jax
import jax.numpy as jnp
from jax import lax
from jax.experimental import pallas as pl
from jax.experimental.pallas import tpu as pltpu
from jax.sharding import PartitionSpec as P

QK_DIM = 64
DA_VAL = 128
HG = 128
BLOCK = 128
KEY_CHUNK = 1024
TAIL = 16
EPSILON = 1e-06
F32 = jnp.float32
BF16 = jnp.bfloat16
NT = (((1,), (1,)), ((), ()))
TN = (((0,), (0,)), ((), ()))


def dot(a, b, dims=(((1,), (0,)), ((), ())), precision=None):
    return lax.dot_general(a, b, dims, precision=precision, preferred_element_type=F32)


def kernel(
    line, tp_count, feats,
    tokens, gain, lam, attn_gain, gap, extra, init, rec_gain,
    w0, w1, w2, w3, w4, w5, w6, wa, wr,
    out,
    tok, sums, wbuf, wobuf, acc, kv, pq, rec_local, qdec, mine, other, pair_f, pair_b,
    partial, parts,
    w_sem, t_send, t_recv, up_send, up_recv, dn_send, dn_recv, x_send, x_recv,
    s_send, s_recv, su_send, su_recv, sd_send, sd_recv, o_send, o_recv,
):
    rows, fb = tokens.shape
    width = w0.shape[1]
    heads = width // HG
    sp = lax.axis_index("sp")
    tp = lax.axis_index("tp")
    z = sp // 2
    x = sp % 2
    sp_x = z * 2 + (1 - x)
    tp1 = tp + 1 - 2 * (tp % 2)
    tp2 = (tp + 2) % 4
    tp3 = 3 - tp
    has_up = z + 1 < line
    has_dn = z >= 1

    def dev(s, t):
        return (s, t)

    def remote(src, dst, ss, rs, to):
        return pltpu.make_async_remote_copy(
            src_ref=src, dst_ref=dst, send_sem=ss, recv_sem=rs,
            device_id=to, device_id_type=pl.DeviceIdType.MESH,
        )

    order = (1, 2, 0, 3, 4, 5, 6)
    weights = (w0, w1, w2, w3, w4, w5, w6)
    loads = {}
    for w in order:
        loads[w] = pltpu.make_async_copy(weights[w], wbuf.at[w], w_sem.at[w])
        loads[w].start()
    load_a = pltpu.make_async_copy(wa, wobuf.at[0], w_sem.at[7])
    load_r = pltpu.make_async_copy(wr, wobuf.at[1], w_sem.at[8])
    load_a.start()
    load_r.start()

    barrier = pltpu.get_barrier_semaphore()
    for t in (tp1, tp2, tp3):
        pl.semaphore_signal(barrier, inc=1, device_id=dev(sp, t), device_id_type=pl.DeviceIdType.MESH)
    pl.semaphore_signal(barrier, inc=1, device_id=dev(sp_x, tp), device_id_type=pl.DeviceIdType.MESH)

    @pl.when(has_up)
    def _():
        pl.semaphore_signal(barrier, inc=1, device_id=dev(sp + 2, tp), device_id_type=pl.DeviceIdType.MESH)

    @pl.when(has_dn)
    def _():
        pl.semaphore_signal(barrier, inc=1, device_id=dev(sp - 2, tp), device_id_type=pl.DeviceIdType.MESH)

    pl.semaphore_wait(barrier, 4 + has_up.astype(jnp.int32) + has_dn.astype(jnp.int32))

    to_y = remote(tokens, tok.at[tp], t_send.at[0], t_recv.at[0], dev(sp, tp2))
    to_1 = remote(tokens, tok.at[tp], t_send.at[1], t_recv.at[1], dev(sp, tp1))
    on_1 = remote(tok.at[tp2], tok.at[tp2], t_send.at[2], t_recv.at[2], dev(sp, tp1))
    to_y.start()
    to_1.start()

    def scaled_of(ref, owner):
        v = ref[...].astype(F32)
        sq = jnp.sum(v * v, axis=1, keepdims=True)
        g = gain[0:1, pl.ds(pl.multiple_of(owner * fb, fb), fb)]
        return (v * g).astype(BF16), sq

    def product(s, owner, w):
        return dot(s, wbuf[w, pl.ds(pl.multiple_of(owner * fb, fb), fb), :])

    def col(w):
        return slice(w * width, (w + 1) * width)

    s, sq0 = scaled_of(tokens, tp)
    for w in order:
        loads[w].wait()
        acc[:, col(w)] = product(s, tp, w)
    to_1.wait_recv()
    s, sq1 = scaled_of(tok.at[tp1], tp1)
    for w in order:
        acc[:, col(w)] += product(s, tp1, w)
    to_y.wait_recv()
    on_1.start()
    s, sq2 = scaled_of(tok.at[tp2], tp2)
    for w in order:
        acc[:, col(w)] += product(s, tp2, w)
    on_1.wait_recv()
    s, sq3 = scaled_of(tok.at[tp3], tp3)
    inv = lax.rsqrt((sq0 + sq1 + sq2 + sq3) / feats + EPSILON)

    def project(w):
        return ((acc[:, col(w)] + product(s, tp3, w)) * inv).astype(BF16)

    kv[sp, :, :width] = project(1)
    kv[sp, :, width:] = project(2)

    def up(h):
        slot = sp - 2 * (h - 1)
        return remote(kv.at[slot], kv.at[slot], up_send.at[h], up_recv.at[h], dev(sp + 2, tp))

    def dn(h):
        slot = sp + 2 * (h - 1)
        return remote(kv.at[slot], kv.at[slot], dn_send.at[h], dn_recv.at[h], dev(sp - 2, tp))

    def across(slot, k):
        return remote(kv.at[slot], kv.at[slot], x_send.at[k], x_recv.at[k], dev(sp_x, tp))

    pl.when(has_up)(lambda: up(1).start())
    pl.when(has_dn)(lambda: dn(1).start())
    across(sp, 0).start()

    pq[...] = (project(0).astype(F32) * QK_DIM ** -0.5).astype(BF16)
    rq = project(3).astype(F32)
    forgets = (project(4).astype(F32), project(5).astype(F32))
    rv = project(6)
    q_all = rq / (1.0 + jnp.exp(-rq)) * HG ** -0.5

    blocks = rows // BLOCK
    r_id = lax.broadcasted_iota(jnp.int32, (BLOCK, BLOCK), 0)
    c_id = lax.broadcasted_iota(jnp.int32, (BLOCK, BLOCK), 1)
    for d in range(2):
        mask = c_id <= r_id if d == 0 else c_id >= r_id
        tri = mask.astype(F32)
        key_all = gap[d : d + 1, :] / (1.0 + jnp.exp(forgets[d]))
        lg_all = jnp.log1p(-key_all)
        states = [None] * heads
        totals = [None] * heads
        for b in range(blocks) if d == 0 else reversed(range(blocks)):
            rs = slice(b * BLOCK, (b + 1) * BLOCK)
            for h in range(heads):
                hs = slice(h * HG, (h + 1) * HG)
                g = lg_all[rs, hs] + extra[d, rs, h : h + 1]
                c = dot(tri, g, precision=lax.Precision.HIGHEST)
                end = c[BLOCK - 1 : BLOCK] if d == 0 else c[0:1]
                mid = end * 0.5
                q = q_all[rs, hs]
                k = key_all[rs, hs]
                v = rv[rs, hs]
                scores = dot((q * jnp.exp(c - mid)).astype(BF16), (k * jnp.exp(mid - c)).astype(BF16), NT)
                scores = jnp.where(mask, scores, 0.0).astype(BF16)
                res = dot(scores, v)
                add = dot(v, (k * jnp.exp(end - c)).astype(BF16), TN)
                if states[h] is None:
                    qdec[d, rs, hs] = (q * jnp.exp(c)).astype(BF16)
                    states[h] = add
                    totals[h] = end
                else:
                    res = res + dot((q * jnp.exp(c)).astype(BF16), states[h].astype(BF16), NT)
                    qdec[d, rs, hs] = (q * jnp.exp(c + totals[h])).astype(BF16)
                    states[h] = states[h] * jnp.exp(end) + add
                    totals[h] = totals[h] + end
                if d == 0:
                    rec_local[rs, hs] = res
                else:
                    rec_local[rs, hs] += res
        store_state(mine.at[d], states, totals, heads)

    swap = remote(mine, other, s_send.at[0], s_recv.at[0], dev(sp_x, tp))
    swap.start()

    def receive(h):
        @pl.when(z >= h)
        def _():
            up(h).wait_recv()
            pl.when(has_up)(lambda: up(h + 1).start())
            across(sp - 2 * h, h).start()

        @pl.when(z + h < line)
        def _():
            dn(h).wait_recv()
            pl.when(has_dn)(lambda: dn(h + 1).start())
            across(sp + 2 * h, line - 1 + h).start()

    if line > 1:
        receive(1)

    swap.wait_recv()
    for d in range(2):
        s_mine, l_mine = load_state(mine.at[d], heads)
        s_other, l_other = load_state(other.at[d], heads)
        first_is_mine = x == d
        pairs, logs = [], []
        for h in range(heads):
            early = jnp.where(first_is_mine, s_mine[h], s_other[h])
            late = jnp.where(first_is_mine, s_other[h], s_mine[h])
            l_late = jnp.where(first_is_mine, l_other[h], l_mine[h])
            pairs.append(early * jnp.exp(l_late) + late)
            logs.append(l_mine[h] + l_other[h])
        store_state((pair_f if d == 0 else pair_b).at[z], pairs, logs, heads)

    def s_up(h):
        slot = z - (h - 1)
        return remote(pair_f.at[slot], pair_f.at[slot], su_send.at[h], su_recv.at[h], dev(sp + 2, tp))

    def s_dn(h):
        slot = z + (h - 1)
        return remote(pair_b.at[slot], pair_b.at[slot], sd_send.at[h], sd_recv.at[h], dev(sp - 2, tp))

    pl.when(has_up)(lambda: s_up(1).start())
    pl.when(has_dn)(lambda: s_dn(1).start())

    for h in range(1, line):
        if h > 1:
            receive(h)

        @pl.when(z >= h)
        def _(h=h):
            s_up(h).wait_recv()
            pl.when(has_up)(lambda: s_up(h + 1).start())

        @pl.when(z + h < line)
        def _(h=h):
            s_dn(h).wait_recv()
            pl.when(has_dn)(lambda: s_dn(h + 1).start())

    for d in range(2):
        buf = pair_f if d == 0 else pair_b

        def fold(i, carry, d=d, buf=buf):
            st, lg = load_state(buf.at[i if d == 0 else line - 1 - i], heads)
            return tuple(carry[h] * jnp.exp(lg[h]) + st[h] for h in range(heads))

        start = tuple(init[d, h].T for h in range(heads))
        enter = lax.fori_loop(0, z if d == 0 else line - 1 - z, fold, start)
        st, lg = load_state(other.at[d], heads)
        for h in range(heads):
            hs = slice(h * HG, (h + 1) * HG)
            e = jnp.where(x == 1 - d, enter[h] * jnp.exp(lg[h]) + st[h], enter[h])
            rec_local[:, hs] += dot(qdec[d, :, hs], e.astype(BF16), NT)
    rec_out = []
    for h in range(heads):
        r = rec_local[:, h * HG : (h + 1) * HG]
        n = r * lax.rsqrt(jnp.mean(r * r, axis=1, keepdims=True) + EPSILON) * rec_gain[...]
        rec_out.append(n.astype(BF16))

    across(sp, 0).wait_recv()
    for h in range(1, line):
        pl.when(z >= h)(lambda h=h: across(sp - 2 * h, h).wait_recv())
        pl.when(z + h < line)(lambda h=h: across(sp + 2 * h, line - 1 + h).wait_recv())

    slots = 2 * line
    per = max(c for c in range(1, slots + 1) if slots % c == 0 and c * rows <= max(KEY_CHUNK, rows))
    attn_out = []
    lane = lax.broadcasted_iota(jnp.int32, (rows, DA_VAL), 1)
    for h in range(heads):
        hs = slice(h * DA_VAL, (h + 1) * DA_VAL)
        vs = slice(width + h * DA_VAL, width + (h + 1) * DA_VAL)
        q = pq[:, hs].astype(F32)
        q = jnp.concatenate(
            [jnp.where(lane < QK_DIM, q, 0.0), jnp.where(lane >= QK_DIM, q, 0.0)], axis=0
        ).astype(BF16)

        def part(i, q=q, hs=hs, vs=vs):
            block = pl.ds(i * per, per)
            k = kv[block, :, hs].reshape(per * rows, DA_VAL)
            v = kv[block, :, vs].reshape(per * rows, DA_VAL)
            sc = dot(q, k, NT)
            m = jnp.max(sc, axis=1, keepdims=True)
            e = jnp.exp(sc - m)
            return m, jnp.sum(e, axis=1, keepdims=True), dot(e.astype(BF16), v)

        def absorb(i, carry, part=part):
            m0, d0, n0 = carry
            m1, d1, n1 = part(i)
            m = jnp.maximum(m0, m1)
            f0, f1 = jnp.exp(m0 - m), jnp.exp(m1 - m)
            return m, d0 * f0 + d1 * f1, n0 * f0 + n1 * f1

        carry = part(0)
        if slots // per > 1:
            carry = lax.fori_loop(1, slots // per, absorb, carry)
        ratio = carry[2] / carry[1]
        diff = ratio[:rows] - lam[0, h] * ratio[rows:]
        n = diff * lax.rsqrt(jnp.mean(diff * diff, axis=1, keepdims=True) + EPSILON) * attn_gain[...]
        attn_out.append(n.astype(BF16))

    load_a.wait()
    load_r.wait()
    a_all = jnp.concatenate(attn_out, axis=1)
    r_all = jnp.concatenate(rec_out, axis=1)
    own = rows // tp_count
    chunks = partial.shape[0]
    cw = partial.shape[2]
    peers = (tp3, tp2, tp1)

    def send(j, i):
        return remote(
            partial.at[j, pl.ds(pl.multiple_of(peers[i] * own, own), own)], parts.at[j, i],
            o_send.at[3 * j + i], o_recv.at[3 * j + i], dev(sp, peers[i]),
        )

    for j in range(chunks):
        cs = slice(j * cw, (j + 1) * cw)
        partial[j] = (dot(a_all, wobuf[0, :, cs]) + dot(r_all, wobuf[1, :, cs])).astype(BF16)
        for i in range(3):
            send(j, i).start()
    mine_rows = pl.ds(pl.multiple_of(tp * own, own), own)
    for j in range(chunks):
        total = partial[j, mine_rows, :].astype(F32)
        for i in range(3):
            send(j, i).wait_recv()
            total = total + parts[j, i].astype(F32)
        out[:, j * cw : (j + 1) * cw] = total.astype(BF16)

    to_y.wait_send()
    to_1.wait_send()
    on_1.wait_send()
    swap.wait_send()
    across(sp, 0).wait_send()
    for h in range(1, line):
        @pl.when(jnp.logical_and(has_up, z >= h - 1))
        def _(h=h):
            up(h).wait_send()
            s_up(h).wait_send()

        @pl.when(jnp.logical_and(has_dn, z + h - 1 < line))
        def _(h=h):
            dn(h).wait_send()
            s_dn(h).wait_send()

        pl.when(z >= h)(lambda h=h: across(sp - 2 * h, h).wait_send())
        pl.when(z + h < line)(lambda h=h: across(sp + 2 * h, line - 1 + h).wait_send())
    for j in range(chunks):
        for i in range(3):
            send(j, i).wait_send()


def store_state(ref, states, logs, heads):
    for h in range(heads):
        ref[h * HG : (h + 1) * HG, :] = states[h].astype(BF16)
    high = [l.astype(BF16).astype(F32) for l in logs]
    low = [l - hi for l, hi in zip(logs, high)]
    row = lax.broadcasted_iota(jnp.int32, (TAIL, HG), 0)
    tail = jnp.zeros((TAIL, HG), F32)
    for i, value in enumerate(high + low):
        tail = jnp.where(row == i, value, tail)
    ref[heads * HG : heads * HG + TAIL, :] = tail.astype(BF16)


def load_state(ref, heads):
    states = [ref[h * HG : (h + 1) * HG, :].astype(F32) for h in range(heads)]
    tail = ref[heads * HG : heads * HG + TAIL, :].astype(F32)
    logs = [tail[h : h + 1] + tail[heads + h : heads + h + 1] for h in range(heads)]
    return states, logs


def solution(mesh):
    sp_count = mesh.shape["sp"]
    tp_count = mesh.shape["tp"]
    line = sp_count // 2

    def local(
        tokens, norm_gain, da_query, da_key, da_value, mix_lambda, attn_gain,
        rec_query, rec_forget_fwd, rec_forget_bwd, rec_value,
        gate_gap, extra_decay, init_state, rec_gain, out_attn, out_rec,
    ):
        rows, fb = tokens.shape
        feats, width = da_query.shape
        heads = width // HG
        columns = out_attn.shape[1]
        own = rows // tp_count
        chunks = 4
        cw = columns // chunks
        state = (heads * HG + TAIL, HG)
        vm = pl.BlockSpec(memory_space=pltpu.VMEM)
        sm = pl.BlockSpec(memory_space=pltpu.SMEM)
        hb = pl.BlockSpec(memory_space=pl.ANY)
        dma = pltpu.SemaphoreType.DMA
        return pl.pallas_call(
            functools.partial(kernel, line, tp_count, feats),
            out_shape=jax.ShapeDtypeStruct((own, columns), BF16),
            in_specs=[vm, vm, sm, vm, vm, vm, vm, vm] + [hb] * 9,
            out_specs=vm,
            scratch_shapes=[
                pltpu.VMEM((tp_count, rows, fb), BF16),
                pltpu.VMEM((8, 128), F32),
                pltpu.VMEM((7, feats, width), BF16),
                pltpu.VMEM((2, width, columns), BF16),
                pltpu.VMEM((rows, 7 * width), F32),
                pltpu.VMEM((sp_count, rows, 2 * width), BF16),
                pltpu.VMEM((rows, width), BF16),
                pltpu.VMEM((rows, width), F32),
                pltpu.VMEM((2, rows, width), BF16),
                pltpu.VMEM((2,) + state, BF16),
                pltpu.VMEM((2,) + state, BF16),
                pltpu.VMEM((line,) + state, BF16),
                pltpu.VMEM((line,) + state, BF16),
                pltpu.VMEM((chunks, rows, cw), BF16),
                pltpu.VMEM((chunks, 3, own, cw), BF16),
                dma((9,)), dma((3,)), dma((3,)),
                dma((line + 1,)), dma((line + 1,)), dma((line + 1,)), dma((line + 1,)),
                dma((2 * line,)), dma((2 * line,)),
                dma((1,)), dma((1,)),
                dma((line + 1,)), dma((line + 1,)), dma((line + 1,)), dma((line + 1,)),
                dma((3 * chunks,)), dma((3 * chunks,)),
            ],
            compiler_params=pltpu.CompilerParams(
                collective_id=0, has_side_effects=True, vmem_limit_bytes=60 * 1024 * 1024
            ),
        )(
            tokens, norm_gain.reshape(1, -1), mix_lambda.reshape(1, -1), attn_gain.reshape(1, -1),
            gate_gap, extra_decay, init_state, rec_gain.reshape(1, -1),
            da_query, da_key, da_value, rec_query, rec_forget_fwd, rec_forget_bwd, rec_value,
            out_attn, out_rec,
        )

    placed = (
        P("sp", "tp"), P(), P(None, "tp"), P(None, "tp"), P(None, "tp"), P("tp"), P(),
        P(None, "tp"), P(None, "tp"), P(None, "tp"), P(None, "tp"), P(None, "tp"),
        P(None, "sp", "tp"), P(None, "tp", None, None), P(), P("tp", None), P("tp", None),
    )
    return jax.shard_map(
        local, mesh=mesh, in_specs=placed, out_specs=P(("sp", "tp"), None), check_vma=False
    )
```

```python
import functools

import jax
import jax.numpy as jnp
from jax import lax
from jax.experimental import pallas as pl
from jax.experimental.pallas import tpu as pltpu
from jax.sharding import PartitionSpec as P

QK_DIM = 64
DA_VAL = 128
HG = 128
BLOCK = 128
KEY_CHUNK = 1024
TAIL = 16
EPSILON = 1e-06
F32 = jnp.float32
BF16 = jnp.bfloat16
NT = (((1,), (1,)), ((), ()))
TN = (((0,), (0,)), ((), ()))


def dot(a, b, dims=(((1,), (0,)), ((), ())), precision=None):
    return lax.dot_general(a, b, dims, precision=precision, preferred_element_type=F32)


def kernel(
    line, tp_count, feats,
    tokens, gain_h, lam, attn_gain_h, gap_h, extra_h, init_h, rec_gain_h,
    w0, w1, w2, w3, w4, w5, w6, wa, wr,
    out,
    gain, attn_gain, gap, extra, init, rec_gain, tok, wbuf, wobuf, acc, kv, pq, rec_local, qdec, mine, other, pair_f, pair_b,
    partial, parts,
    in_sem, w_sem, t_send, t_recv, up_send, up_recv, dn_send, dn_recv, x_send, x_recv,
    s_send, s_recv, su_send, su_recv, sd_send, sd_recv, o_send, o_recv,
):
    rows, fb = tokens.shape
    width = w0.shape[1]
    heads = width // HG
    sp = lax.axis_index("sp")
    tp = lax.axis_index("tp")
    z = sp // 2
    x = sp % 2
    sp_x = z * 2 + (1 - x)
    tp1 = tp + 1 - 2 * (tp % 2)
    tp2 = (tp + 2) % 4
    tp3 = 3 - tp
    has_up = z + 1 < line
    has_dn = z >= 1

    def dev(s, t):
        return (s, t)

    def remote(src, dst, ss, rs, to):
        return pltpu.make_async_remote_copy(
            src_ref=src, dst_ref=dst, send_sem=ss, recv_sem=rs,
            device_id=to, device_id_type=pl.DeviceIdType.MESH,
        )

    load_t = pltpu.make_async_copy(tokens, tok.at[tp], in_sem.at[0])
    load_t.start()
    smalls = []
    pairs_in = ((gain_h, gain), (extra_h, extra), (gap_h, gap), (init_h, init), (attn_gain_h, attn_gain), (rec_gain_h, rec_gain))
    for i, (a, b) in enumerate(pairs_in):
        smalls.append(pltpu.make_async_copy(a, b, in_sem.at[i + 1]))
    smalls[0].start()
    order = (1, 2, 0, 3, 4, 5, 6)
    weights = (w0, w1, w2, w3, w4, w5, w6)
    loads = {}
    for w in order:
        loads[w] = pltpu.make_async_copy(weights[w], wbuf.at[w], w_sem.at[w])
        loads[w].start()
    load_a = pltpu.make_async_copy(wa, wobuf.at[0], w_sem.at[7])
    load_r = pltpu.make_async_copy(wr, wobuf.at[1], w_sem.at[8])
    load_a.start()
    load_r.start()
    for c in smalls[1:]:
        c.start()

    barrier = pltpu.get_barrier_semaphore()
    for t in (tp1, tp2, tp3):
        pl.semaphore_signal(barrier, inc=1, device_id=dev(sp, t), device_id_type=pl.DeviceIdType.MESH)
    pl.semaphore_signal(barrier, inc=1, device_id=dev(sp_x, tp), device_id_type=pl.DeviceIdType.MESH)
    for h in range(1, line):
        other_z = lax.rem(z + h, line)
        pl.semaphore_signal(
            barrier, inc=1, device_id=dev(other_z * 2 + x, tp), device_id_type=pl.DeviceIdType.MESH
        )
    load_t.wait()
    pl.semaphore_wait(barrier, 4 + line - 1)

    to_y = remote(tok.at[tp], tok.at[tp], t_send.at[0], t_recv.at[0], dev(sp, tp2))
    to_1 = remote(tok.at[tp], tok.at[tp], t_send.at[1], t_recv.at[1], dev(sp, tp1))
    on_1 = remote(tok.at[tp2], tok.at[tp2], t_send.at[2], t_recv.at[2], dev(sp, tp1))
    to_y.start()
    to_1.start()

    def scaled_of(ref, owner):
        v = ref[...].astype(F32)
        sq = jnp.sum(v * v, axis=1, keepdims=True)
        g = gain[0:1, pl.ds(pl.multiple_of(owner * fb, fb), fb)]
        return (v * g).astype(BF16), sq

    def product(s, owner, w):
        return dot(s, wbuf[w, pl.ds(pl.multiple_of(owner * fb, fb), fb), :])

    def col(w):
        return slice(w * width, (w + 1) * width)

    smalls[0].wait()
    s, sq0 = scaled_of(tok.at[tp], tp)
    for w in order:
        loads[w].wait()
        acc[:, col(w)] = product(s, tp, w)
    to_1.wait_recv()
    s, sq1 = scaled_of(tok.at[tp1], tp1)
    for w in order:
        acc[:, col(w)] += product(s, tp1, w)
    to_y.wait_recv()
    on_1.start()
    s, sq2 = scaled_of(tok.at[tp2], tp2)
    for w in order:
        acc[:, col(w)] += product(s, tp2, w)
    on_1.wait_recv()
    s, sq3 = scaled_of(tok.at[tp3], tp3)
    inv = lax.rsqrt((sq0 + sq1 + sq2 + sq3) / feats + EPSILON)

    def project(w):
        return ((acc[:, col(w)] + product(s, tp3, w)) * inv).astype(BF16)

    def up(p, h):
        slot = sp - 2 * (h - 1)
        i = p * (line + 1) + h
        return remote(kv.at[p, slot], kv.at[p, slot], up_send.at[i], up_recv.at[i], dev(sp + 2, tp))

    def dn(p, h):
        slot = sp + 2 * (h - 1)
        i = p * (line + 1) + h
        return remote(kv.at[p, slot], kv.at[p, slot], dn_send.at[i], dn_recv.at[i], dev(sp - 2, tp))

    def across(p, slot, k):
        i = p * 2 * line + k
        return remote(kv.at[p, slot], kv.at[p, slot], x_send.at[i], x_recv.at[i], dev(sp_x, tp))

    for p in range(2):
        kv[p, sp] = project(1 + p)
        pl.when(has_up)(lambda: up(p, 1).start())
        pl.when(has_dn)(lambda: dn(p, 1).start())
        if p == 0:
            across(0, sp, 0).start()

    pq[...] = (project(0).astype(F32) * QK_DIM ** -0.5).astype(BF16)
    rq = project(3).astype(F32)
    forgets = (project(4).astype(F32), project(5).astype(F32))
    rv = project(6)
    q_all = rq / (1.0 + jnp.exp(-rq)) * HG ** -0.5

    for c in smalls[1:]:
        c.wait()
    blocks = rows // BLOCK
    r_id = lax.broadcasted_iota(jnp.int32, (BLOCK, BLOCK), 0)
    c_id = lax.broadcasted_iota(jnp.int32, (BLOCK, BLOCK), 1)
    for d in range(2):
        mask = c_id <= r_id if d == 0 else c_id >= r_id
        tri = mask.astype(F32)
        key_all = gap[d : d + 1, :] / (1.0 + jnp.exp(forgets[d]))
        lg_all = jnp.log1p(-key_all)
        states = [None] * heads
        totals = [None] * heads
        for b in range(blocks) if d == 0 else reversed(range(blocks)):
            rs = slice(b * BLOCK, (b + 1) * BLOCK)
            for h in range(heads):
                hs = slice(h * HG, (h + 1) * HG)
                g = lg_all[rs, hs] + jnp.broadcast_to(extra[d, h : h + 1, rs], (HG, BLOCK)).T
                c = dot(tri, g, precision=lax.Precision.HIGHEST)
                end = c[BLOCK - 1 : BLOCK] if d == 0 else c[0:1]
                mid = end * 0.5
                q = q_all[rs, hs]
                k = key_all[rs, hs]
                v = rv[rs, hs]
                scores = dot((q * jnp.exp(c - mid)).astype(BF16), (k * jnp.exp(mid - c)).astype(BF16), NT)
                scores = jnp.where(mask, scores, 0.0).astype(BF16)
                res = dot(scores, v)
                add = dot(v, (k * jnp.exp(end - c)).astype(BF16), TN)
                if states[h] is None:
                    qdec[d, rs, hs] = (q * jnp.exp(c)).astype(BF16)
                    states[h] = add
                    totals[h] = end
                else:
                    res = res + dot((q * jnp.exp(c)).astype(BF16), states[h].astype(BF16), NT)
                    qdec[d, rs, hs] = (q * jnp.exp(c + totals[h])).astype(BF16)
                    states[h] = states[h] * jnp.exp(end) + add
                    totals[h] = totals[h] + end
                if d == 0:
                    rec_local[rs, hs] = res
                else:
                    rec_local[rs, hs] += res
        store_state(mine.at[d], states, totals, heads)

    swap = remote(mine, other, s_send.at[0], s_recv.at[0], dev(sp_x, tp))
    swap.start()
    across(1, sp, 0).start()

    def receive(h):
        for p in range(2):
            @pl.when(z >= h)
            def _(p=p):
                up(p, h).wait_recv()
                pl.when(has_up)(lambda: up(p, h + 1).start())
                across(p, sp - 2 * h, h).start()

            @pl.when(z + h < line)
            def _(p=p):
                dn(p, h).wait_recv()
                pl.when(has_dn)(lambda: dn(p, h + 1).start())
                across(p, sp + 2 * h, line - 1 + h).start()

    if line > 1:
        receive(1)

    swap.wait_recv()
    for d in range(2):
        s_mine, l_mine = load_state(mine.at[d], heads)
        s_other, l_other = load_state(other.at[d], heads)
        first_is_mine = x == d
        pairs, logs = [], []
        for h in range(heads):
            early = jnp.where(first_is_mine, s_mine[h], s_other[h])
            late = jnp.where(first_is_mine, s_other[h], s_mine[h])
            l_late = jnp.where(first_is_mine, l_other[h], l_mine[h])
            pairs.append(early * jnp.exp(l_late) + late)
            logs.append(l_mine[h] + l_other[h])
        store_state((pair_f if d == 0 else pair_b).at[z], pairs, logs, heads)

    def s_up(slot, h):
        return remote(pair_f.at[slot], pair_f.at[slot], su_send.at[h], su_recv.at[h], dev(sp + 2 * h, tp))

    def s_dn(slot, h):
        return remote(pair_b.at[slot], pair_b.at[slot], sd_send.at[h], sd_recv.at[h], dev(sp - 2 * h, tp))

    for h in range(1, line):
        pl.when(z + h < line)(lambda h=h: s_up(z, h).start())
        pl.when(z >= h)(lambda h=h: s_dn(z, h).start())
    for h in range(2, line):
        receive(h)
    for h in range(1, line):
        pl.when(z >= h)(lambda h=h: s_up(z - h, h).wait_recv())
        pl.when(z + h < line)(lambda h=h: s_dn(z + h, h).wait_recv())

    for d in range(2):
        buf = pair_f if d == 0 else pair_b

        def fold(i, carry, d=d, buf=buf):
            st, lg = load_state(buf.at[i if d == 0 else line - 1 - i], heads)
            return tuple(carry[h] * jnp.exp(lg[h]) + st[h] for h in range(heads))

        start = tuple(init[d, h].T for h in range(heads))
        enter = lax.fori_loop(0, z if d == 0 else line - 1 - z, fold, start)
        st, lg = load_state(other.at[d], heads)
        for h in range(heads):
            hs = slice(h * HG, (h + 1) * HG)
            e = jnp.where(x == 1 - d, enter[h] * jnp.exp(lg[h]) + st[h], enter[h])
            rec_local[:, hs] += dot(qdec[d, :, hs], e.astype(BF16), NT)
    rec_out = []
    for h in range(heads):
        r = rec_local[:, h * HG : (h + 1) * HG]
        n = r * lax.rsqrt(jnp.mean(r * r, axis=1, keepdims=True) + EPSILON) * rec_gain[...]
        rec_out.append(n.astype(BF16))

    for p in range(2):
        across(p, sp, 0).wait_recv()
        for h in range(1, line):
            pl.when(z >= h)(lambda: across(p, sp - 2 * h, h).wait_recv())
            pl.when(z + h < line)(lambda: across(p, sp + 2 * h, line - 1 + h).wait_recv())

    slots = 2 * line
    per = max(c for c in range(1, slots + 1) if slots % c == 0 and c * rows <= max(KEY_CHUNK, rows))
    attn_out = []
    lane = lax.broadcasted_iota(jnp.int32, (rows, DA_VAL), 1)
    for h in range(heads):
        hs = slice(h * DA_VAL, (h + 1) * DA_VAL)
        q = pq[:, hs].astype(F32)
        q = jnp.concatenate(
            [jnp.where(lane < QK_DIM, q, 0.0), jnp.where(lane >= QK_DIM, q, 0.0)], axis=0
        ).astype(BF16)

        def part(i, q=q, hs=hs):
            block = pl.ds(i * per, per)
            k = kv[0, block, :, hs].reshape(per * rows, DA_VAL)
            v = kv[1, block, :, hs].reshape(per * rows, DA_VAL)
            sc = dot(q, k, NT)
            m = jnp.max(sc, axis=1, keepdims=True)
            e = jnp.exp(sc - m)
            return m, jnp.sum(e, axis=1, keepdims=True), dot(e.astype(BF16), v)

        def absorb(i, carry, part=part):
            m0, d0, n0 = carry
            m1, d1, n1 = part(i)
            m = jnp.maximum(m0, m1)
            f0, f1 = jnp.exp(m0 - m), jnp.exp(m1 - m)
            return m, d0 * f0 + d1 * f1, n0 * f0 + n1 * f1

        carry = part(0)
        if slots // per > 1:
            carry = lax.fori_loop(1, slots // per, absorb, carry)
        ratio = carry[2] / carry[1]
        diff = ratio[:rows] - lam[0, h] * ratio[rows:]
        n = diff * lax.rsqrt(jnp.mean(diff * diff, axis=1, keepdims=True) + EPSILON) * attn_gain[...]
        attn_out.append(n.astype(BF16))

    load_a.wait()
    load_r.wait()
    a_all = jnp.concatenate(attn_out, axis=1)
    r_all = jnp.concatenate(rec_out, axis=1)
    own = rows // tp_count
    chunks = partial.shape[0]
    cw = partial.shape[2]
    peers = (tp3, tp2, tp1)

    def send(j, i):
        return remote(
            partial.at[j, pl.ds(pl.multiple_of(peers[i] * own, own), own)], parts.at[j, i],
            o_send.at[3 * j + i], o_recv.at[3 * j + i], dev(sp, peers[i]),
        )

    for j in range(chunks):
        cs = slice(j * cw, (j + 1) * cw)
        partial[j] = (dot(a_all, wobuf[0, :, cs]) + dot(r_all, wobuf[1, :, cs])).astype(BF16)
        for i in range(3):
            send(j, i).start()
    mine_rows = pl.ds(pl.multiple_of(tp * own, own), own)
    for j in range(chunks):
        total = partial[j, mine_rows, :].astype(F32)
        for i in range(3):
            send(j, i).wait_recv()
            total = total + parts[j, i].astype(F32)
        out[:, j * cw : (j + 1) * cw] = total.astype(BF16)

    to_y.wait_send()
    to_1.wait_send()
    on_1.wait_send()
    swap.wait_send()
    for p in range(2):
        across(p, sp, 0).wait_send()
        for h in range(1, line):
            pl.when(jnp.logical_and(has_up, z >= h - 1))(lambda: up(p, h).wait_send())
            pl.when(jnp.logical_and(has_dn, z + h - 1 < line))(lambda: dn(p, h).wait_send())
            pl.when(z >= h)(lambda: across(p, sp - 2 * h, h).wait_send())
            pl.when(z + h < line)(lambda: across(p, sp + 2 * h, line - 1 + h).wait_send())
    for h in range(1, line):
        pl.when(z + h < line)(lambda h=h: s_up(z, h).wait_send())
        pl.when(z >= h)(lambda h=h: s_dn(z, h).wait_send())
    for j in range(chunks):
        for i in range(3):
            send(j, i).wait_send()


def store_state(ref, states, logs, heads):
    for h in range(heads):
        ref[h * HG : (h + 1) * HG, :] = states[h].astype(BF16)
    high = [l.astype(BF16).astype(F32) for l in logs]
    low = [l - hi for l, hi in zip(logs, high)]
    row = lax.broadcasted_iota(jnp.int32, (TAIL, HG), 0)
    tail = jnp.zeros((TAIL, HG), F32)
    for i, value in enumerate(high + low):
        tail = jnp.where(row == i, value, tail)
    ref[heads * HG : heads * HG + TAIL, :] = tail.astype(BF16)


def load_state(ref, heads):
    states = [ref[h * HG : (h + 1) * HG, :].astype(F32) for h in range(heads)]
    tail = ref[heads * HG : heads * HG + TAIL, :].astype(F32)
    logs = [tail[h : h + 1] + tail[heads + h : heads + h + 1] for h in range(heads)]
    return states, logs


def solution(mesh):
    sp_count = mesh.shape["sp"]
    tp_count = mesh.shape["tp"]
    line = sp_count // 2

    def local(
        tokens, norm_gain, da_query, da_key, da_value, mix_lambda, attn_gain,
        rec_query, rec_forget_fwd, rec_forget_bwd, rec_value,
        gate_gap, extra_decay, init_state, rec_gain, out_attn, out_rec,
    ):
        rows, fb = tokens.shape
        feats, width = da_query.shape
        heads = width // HG
        columns = out_attn.shape[1]
        own = rows // tp_count
        chunks = 4
        cw = columns // chunks
        state = (heads * HG + TAIL, HG)
        vm = pl.BlockSpec(memory_space=pltpu.VMEM)
        sm = pl.BlockSpec(memory_space=pltpu.SMEM)
        hb = pl.BlockSpec(memory_space=pltpu.HBM)
        dma = pltpu.SemaphoreType.DMA
        return pl.pallas_call(
            functools.partial(kernel, line, tp_count, feats),
            out_shape=jax.ShapeDtypeStruct((own, columns), BF16),
            in_specs=[hb, hb, sm, hb, hb, hb, hb, hb] + [hb] * 9,
            out_specs=vm,
            scratch_shapes=[
                pltpu.VMEM((1, norm_gain.shape[0]), F32),
                pltpu.VMEM((1, attn_gain.shape[0]), F32),
                pltpu.VMEM(gate_gap.shape, F32),
                pltpu.VMEM((2, heads, rows), F32),
                pltpu.VMEM(init_state.shape, F32),
                pltpu.VMEM((1, rec_gain.shape[0]), F32),
                pltpu.VMEM((tp_count, rows, fb), BF16),
                pltpu.VMEM((7, feats, width), BF16),
                pltpu.VMEM((2, width, columns), BF16),
                pltpu.VMEM((rows, 7 * width), F32),
                pltpu.VMEM((2, sp_count, rows, width), BF16),
                pltpu.VMEM((rows, width), BF16),
                pltpu.VMEM((rows, width), F32),
                pltpu.VMEM((2, rows, width), BF16),
                pltpu.VMEM((2,) + state, BF16),
                pltpu.VMEM((2,) + state, BF16),
                pltpu.VMEM((line,) + state, BF16),
                pltpu.VMEM((line,) + state, BF16),
                pltpu.VMEM((chunks, rows, cw), BF16),
                pltpu.VMEM((chunks, 3, own, cw), BF16),
                dma((7,)), dma((9,)), dma((3,)), dma((3,)),
                dma((2 * line + 2,)), dma((2 * line + 2,)), dma((2 * line + 2,)), dma((2 * line + 2,)),
                dma((4 * line,)), dma((4 * line,)),
                dma((1,)), dma((1,)),
                dma((line + 1,)), dma((line + 1,)), dma((line + 1,)), dma((line + 1,)),
                dma((3 * chunks,)), dma((3 * chunks,)),
            ],
            compiler_params=pltpu.CompilerParams(
                collective_id=0, has_side_effects=True, vmem_limit_bytes=56 * 1024 * 1024
            ),
        )(
            tokens, norm_gain.reshape(1, -1), mix_lambda.reshape(1, -1), attn_gain.reshape(1, -1),
            gate_gap, extra_decay.transpose(0, 2, 1), init_state, rec_gain.reshape(1, -1),
            da_query, da_key, da_value, rec_query, rec_forget_fwd, rec_forget_bwd, rec_value,
            out_attn, out_rec,
        )

    placed = (
        P("sp", "tp"), P(), P(None, "tp"), P(None, "tp"), P(None, "tp"), P("tp"), P(),
        P(None, "tp"), P(None, "tp"), P(None, "tp"), P(None, "tp"), P(None, "tp"),
        P(None, "sp", "tp"), P(None, "tp", None, None), P(), P("tp", None), P("tp", None),
    )
    return jax.shard_map(
        local, mesh=mesh, in_specs=placed, out_specs=P(("sp", "tp"), None), check_vma=False
    )
```
